32 devices in a mesh: ep: 8 (over z, y), tp: 4 (over x, core).
Axes of the slice: x: 2, y: 2, z: 4, core: 2. Of those that a mesh axis runs over, the one named last changes fastest.
Arguments:
- tokens: bfloat16 [64, 2048], P('ep'), may hold values from -4 to 4
- w_query: bfloat16 [2048, 1024], P(None, 'tp'), may hold values from -0.125 to 0.125
- w_key: bfloat16 [2048, 1024], P(None, 'tp'), may hold values from -0.125 to 0.125
- w_value: bfloat16 [2048, 1024], P(None, 'tp'), may hold values from -0.125 to 0.125
- w_outgate: bfloat16 [2048, 1024], P(None, 'tp'), may hold values from -0.125 to 0.125
- w_igate: bfloat16 [2048, 4], P(None, 'tp'), may hold values from -0.125 to 0.125
- w_fgate: bfloat16 [2048, 4], P(None, 'tp'), may hold values from -0.125 to 0.125
- forget_bias: float32 [4], P('tp'), may hold values from -1 to 5
- w_out: bfloat16 [1024, 2048], P('tp'), may hold values from -0.1875 to 0.1875
- gain_mix: float32 [2048], replicated, may hold values from 0.1 to 1.9
- gain_moe: float32 [2048], replicated, may hold values from 0.1 to 1.9
- memory: float32 [64, 4, 256, 256], P('ep', 'tp'), may hold values from -0.4 to 0.4
- normalizer: float32 [64, 4, 256], P('ep', 'tp'), may hold values from -0.8 to 0.8
- stabilizer: float32 [64, 4], P('ep', 'tp'), may hold values from 0 to 2
- expert_gate: bfloat16 [8, 2048, 512], P('ep', None, 'tp'), may hold values from -0.125 to 0.125
- expert_up: bfloat16 [8, 2048, 512], P('ep', None, 'tp'), may hold values from -0.125 to 0.125
- expert_down: bfloat16 [8, 512, 2048], P('ep', 'tp'), may hold values from -1 to 1
- routes: int32 [64, 4], P('ep'), may hold values from 0 to 7, all different within a row; in each aligned block of 8 rows (0 to 7, 8 to 15, ...) at most 8 rows name the same one
- route_weight: float32 [64, 4], P('ep'), may hold values from 0.2 to 1
Outputs:
- output: bfloat16 [64, 2048], P('ep', 'tp')
- memory_next: float32 [64, 4, 256, 256], P('ep', 'tp')
- norm_next: float32 [64, 4, 256], P('ep', 'tp')
- stabilizer_next: float32 [64, 4], P('ep', 'tp')
The draws below stay inside these ranges and needn't reach their ends.
Inputs may be any that keep to these rules, and one draw needn't show every extreme that they name: `routes`: each row names 4 different experts. Among the 8 rows of one device (aligned blocks), no expert is named more than 8 times, a bound that some block reaches.
All inputs are finite; a program needn't handle non-finite values.
Results may differ from the reference program's by a relative error of at most 0.029.
Values may be sent and summed in bfloat16 or wider, within the bound.
A program may use at most 64 MiB of HBM per device.

```python
import math
import jax
import jax.numpy as jnp
import numpy as np
from jax import lax

D = 2048
NH = 4
DH = 256
FF = 512
TOP = 4
SEQ_DEV = 8
TOKENS = 64
EXPERTS = 8
CAP = 8
N_EP = 8


def steps_of(stream_key, shape, pieces, least, high):
    loudness = 1.0
    for position, parts in pieces:
        steps = jax.random.uniform(jax.random.fold_in(jax.random.fold_in(stream_key, 6), position), (parts,), jnp.float32, least / len(pieces), high / len(pieces))
        loudness = loudness * jnp.repeat(jnp.exp(steps), shape[position] // parts).reshape((-1,) + (1,) * (len(shape) - 1 - position))
    return loudness


def routed_block(rng, own, number, rows, count, top, reach, slope):
    order = jax.random.permutation(rng, count)
    crowded, ordinary = load_shares(count, rows * top, reach, slope, True), load_shares(count, rows * top, reach, slope, False)
    places = jnp.arange(count)

    def named(tallies, offset_by):
        used = int((tallies > 0).sum())
        fixed = max(1, used // 4)
        passed = fixed + (places - fixed + offset_by * (used - fixed)) % max(1, count - fixed)
        return jnp.zeros((count,), jnp.int32).at[order[jnp.where(places < fixed, places, passed)]].set(jnp.asarray(tallies, jnp.int32))

    tallies = jnp.where(number % 4 == 0, named(crowded, number // 4), named(ordinary, number - number // 4 - 1))
    mixed = jax.random.permutation(jax.random.fold_in(own, 3), count)
    giver, sink = mixed[0:count // 2 * 2:2], mixed[1:count // 2 * 2:2]
    margin = jnp.minimum(tallies[giver] - 1, reach - tallies[sink]) // 2
    margin = jnp.where((giver == order[0]) | (sink == order[0]) | (tallies[sink] == 0), 0, jnp.maximum(margin, 0))
    passed = jax.random.randint(jax.random.fold_in(own, 4), (count // 2,), 0, 1 << 20) % (margin + 1)
    tallies = tallies.at[giver].add(-passed).at[sink].add(passed)
    items = jnp.searchsorted(jnp.cumsum(tallies), jnp.arange(rows * top), side="right").astype(jnp.int32)
    grid = items.reshape(top, rows).T
    grid = grid[jax.random.permutation(jax.random.fold_in(own, 1), rows)]
    offset_by = jax.random.randint(jax.random.fold_in(own, 2), (rows, 1), 0, top)
    return jnp.take_along_axis(grid, (jnp.arange(top)[None, :] + offset_by) % top, axis=1)


def load_shares(count, total, reach, slope, full):
    loads = [(1 << 20) // math.isqrt(standing ** slope) + 1 for standing in range(1, count + 1)]
    largest = reach if full else min(reach, max(-(-total // count), total * loads[0] // sum(loads)))
    least = 1 if total - largest >= count - 1 else 0
    counts, spare = [largest] + [least] * (count - 1), total - largest - least * (count - 1)
    while spare > 0:
        free = [i for i in range(1, count) if counts[i] < largest] or [i for i in range(1, count) if counts[i] < reach]
        mass, left = sum([loads[i] for i in free]), spare
        for i in free:
            more = min(reach - counts[i], max(1, left * loads[i] // mass), spare)
            counts[i] = counts[i] + more
            spare = spare - more
    return np.array(counts)


def scatter_about(stream_key, extent, deviation, reach, split=(), held_as=jnp.bfloat16):
    values = jax.random.normal(stream_key, extent, jnp.float32) * deviation
    if len(split) > 0:
        values = steps_of(stream_key, extent, split, -0.22, 0.18) * values
    return jnp.clip(values, min=-reach, max=reach).astype(held_as)


def setup_inputs(seed: int = 0) -> dict:
    key_list = jax.random.split(jax.random.key(seed), 20)
    tokens = scatter_about(key_list[0], (TOKENS, D), 1.0, 4.0, ((0, 8),))
    w_query = scatter_about(key_list[1], (D, NH * DH), D ** -0.5, 0.125, ((1, 4),))
    w_key = scatter_about(key_list[2], (D, NH * DH), D ** -0.5, 0.125, ((1, 4),))
    w_value = scatter_about(key_list[3], (D, NH * DH), D ** -0.5, 0.125, ((1, 4),))
    w_outgate = scatter_about(key_list[4], (D, NH * DH), D ** -0.5, 0.125, ((1, 4),))
    w_igate = scatter_about(key_list[5], (D, NH), D ** -0.5, 0.125, ((1, 4),))
    w_fgate = scatter_about(key_list[6], (D, NH), D ** -0.5, 0.125, ((1, 4),))
    forget_bias = jnp.clip(-1.0 + 6.0 * jax.random.uniform(key_list[7], (NH,), jnp.float32) ** steps_of(key_list[7], (NH,), ((0, 4),), -0.2, 0.2), -1.0, 5.0)
    w_out = scatter_about(key_list[8], (NH * DH, D), (NH * DH) ** -0.5, 0.1875, ((0, 4),))
    gain_mix = jnp.clip(1.0 + 0.18 * jax.random.normal(key_list[9], (D,), jnp.float32), 0.1, 1.9)
    gain_moe = jnp.clip(1.0 + 0.18 * jax.random.normal(key_list[10], (D,), jnp.float32), 0.1, 1.9)
    memory = scatter_about(key_list[11], (TOKENS, NH, DH, DH), 0.05, 0.4, ((0, 8), (1, 4)), jnp.float32)
    normalizer = scatter_about(key_list[12], (TOKENS, NH, DH), 0.1, 0.8, ((0, 8), (1, 4)), jnp.float32)
    stabilizer = jnp.clip(2.0 * jax.random.uniform(key_list[13], (TOKENS, NH), jnp.float32) ** steps_of(key_list[13], (TOKENS, NH), ((0, 8), (1, 4)), -0.2, 0.2), 0.0, 2.0)
    expert_gate = scatter_about(key_list[14], (EXPERTS, D, FF), D ** -0.5, 0.125, ((0, 8), (2, 4)))
    expert_up = scatter_about(key_list[15], (EXPERTS, D, FF), D ** -0.5, 0.125, ((0, 8), (2, 4)))
    expert_down = scatter_about(key_list[16], (EXPERTS, FF, D), (FF // 16) ** -0.5, 1.0, ((0, 8), (1, 4)))
    routes_keys = jax.random.split(jax.random.fold_in(key_list[17], 1), TOKENS // SEQ_DEV)
    routes_turns = jax.random.permutation(jax.random.fold_in(key_list[17], 3), TOKENS // SEQ_DEV)
    routes = jax.vmap(lambda own, number: routed_block(jax.random.fold_in(key_list[17], 2), own, number, SEQ_DEV, EXPERTS, TOP, CAP, 2))(routes_keys, routes_turns).reshape((TOKENS, TOP))
    route_weight = jnp.clip(0.2 + 0.8 * jax.random.uniform(key_list[18], (TOKENS, TOP), jnp.float32) ** steps_of(key_list[18], (TOKENS, TOP), ((0, 8),), -0.2, 0.2), 0.2, 1.0)
    return dict(tokens=tokens, w_query=w_query, w_key=w_key, w_value=w_value, w_outgate=w_outgate, w_igate=w_igate, w_fgate=w_fgate, forget_bias=forget_bias, w_out=w_out, gain_mix=gain_mix, gain_moe=gain_moe, memory=memory, normalizer=normalizer, stabilizer=stabilizer, expert_gate=expert_gate, expert_up=expert_up, expert_down=expert_down, routes=routes, route_weight=route_weight)


def layer_norm(row_data, gain_vec):
    values = row_data.astype(jnp.float32)
    row_mean = lax.optimization_barrier(jnp.mean(values, -1, keepdims=True))
    centered = values - row_mean
    variance = lax.optimization_barrier(jnp.mean(centered * centered, -1, keepdims=True))
    return centered * lax.rsqrt(variance + 1e-05) * gain_vec

def slot_targets(routes, experts, capacity):
    flat_routes = routes.reshape(-1)
    onehot = (flat_routes[:, None] == jnp.arange(experts, dtype=jnp.int32)[None, :]).astype(jnp.int32)
    before = jnp.cumsum(onehot, axis=0) - onehot
    slot_index = lax.optimization_barrier(jnp.sum(before * onehot, axis=1))
    return (flat_routes * capacity + slot_index).astype(jnp.int32)

def expert_rows(operands):
    rows_in, gate_weight, up_weight, down_weight = operands
    gate_part = jnp.dot(rows_in, gate_weight, preferred_element_type=jnp.float32)
    up_part = jnp.dot(rows_in, up_weight, preferred_element_type=jnp.float32)
    hidden = (jax.nn.silu(gate_part) * up_part).astype(jnp.bfloat16)
    return jnp.dot(hidden, down_weight, preferred_element_type=jnp.float32).astype(jnp.bfloat16)

def reference(tokens, w_query, w_key, w_value, w_outgate, w_igate, w_fgate, forget_bias, w_out, gain_mix, gain_moe, memory, normalizer, stabilizer, expert_gate, expert_up, expert_down, routes, route_weight):
    normed = layer_norm(tokens, gain_mix).astype(jnp.bfloat16)

    def project(weight):
        rounded = jnp.dot(normed, weight, preferred_element_type=jnp.float32).astype(jnp.bfloat16)
        rounded = lax.optimization_barrier(rounded)
        return rounded.astype(jnp.float32).reshape(TOKENS, NH, DH)
    queries = project(w_query)
    keys_scaled = project(w_key) / math.sqrt(DH)
    values_rows = project(w_value)
    out_gate = project(w_outgate)
    gate_in = jnp.dot(normed, w_igate, preferred_element_type=jnp.float32)
    gate_forget = jnp.dot(normed, w_fgate, preferred_element_type=jnp.float32)
    log_forget = jax.nn.log_sigmoid(gate_forget + forget_bias)
    stabilizer_next = jnp.maximum(log_forget + stabilizer, gate_in)
    keep_rate = jnp.exp(log_forget + stabilizer - stabilizer_next)
    admit_rate = jnp.exp(gate_in - stabilizer_next)
    memory_next = keep_rate[:, :, None, None] * memory + admit_rate[:, :, None, None] * keys_scaled[:, :, :, None] * values_rows[:, :, None, :]
    norm_next = keep_rate[:, :, None] * normalizer + admit_rate[:, :, None] * keys_scaled
    numerator = jnp.einsum('thk,thkv->thv', queries, memory_next, precision=lax.Precision.HIGHEST)
    denominator = lax.optimization_barrier(jnp.sum(queries * norm_next, axis=-1))
    readout = numerator / jnp.maximum(jnp.abs(denominator), jnp.exp(-stabilizer_next))[:, :, None]
    mixed = (jax.nn.sigmoid(out_gate) * readout).astype(jnp.bfloat16)
    head_part = jnp.einsum('thd,hde->the', mixed.astype(jnp.float32), w_out.reshape(NH, DH, D).astype(jnp.float32)).astype(jnp.bfloat16)
    residual = tokens.astype(jnp.float32) + lax.optimization_barrier(jnp.sum(head_part.astype(jnp.float32), axis=1))
    expert_in = layer_norm(residual, gain_moe).astype(jnp.bfloat16)
    blocks = routes.reshape(N_EP, SEQ_DEV * TOP)
    local_target = jax.vmap(lambda route_row: slot_targets(route_row, EXPERTS, CAP))(blocks)
    slot_index = local_target - blocks * CAP
    block_index = jnp.arange(N_EP, dtype=jnp.int32)[:, None]
    placement = ((blocks * N_EP + block_index) * CAP + slot_index).reshape(-1).astype(jnp.int32)
    buffer = jnp.zeros((EXPERTS * N_EP * CAP, D), jnp.bfloat16).at[placement].set(jnp.repeat(expert_in, TOP, axis=0))
    expert_outs = lax.map(expert_rows, (buffer.reshape(EXPERTS, N_EP * CAP, D), expert_gate, expert_up, expert_down))
    picked = expert_outs.reshape(-1, D)[placement].reshape(TOKENS, TOP, D)
    combined = lax.optimization_barrier(jnp.sum(route_weight[:, :, None] * picked.astype(jnp.float32), axis=1))
    output = (residual + combined).astype(jnp.bfloat16)
    return (output, memory_next, norm_next, stabilizer_next)
```

```python
import functools
import math

import jax
import jax.numpy as jnp
from jax import lax
from jax.experimental import pallas as pl
from jax.experimental.pallas import tpu as pltpu
from jax.sharding import PartitionSpec as P

MESH = pl.DeviceIdType.MESH
F32 = jnp.float32
BF16 = jnp.bfloat16


def kernel(
    n_ep,
    n_tp,
    tokens_h,
    gain_mix_h,
    wq_h,
    wk_h,
    wv_h,
    wo_h,
    wi_h,
    wf_h,
    bias_h,
    w_out_h,
    gain_moe_h,
    memory_h,
    normalizer_h,
    stabilizer_h,
    gate_h,
    up_h,
    down_h,
    routes_h,
    weight_h,
    out_ref,
    memory_out,
    norm_out,
    stab_out,
    tokens,
    gain_mix,
    wq,
    wk,
    wv,
    wo,
    wi,
    wf,
    bias,
    w_out,
    gain_moe,
    memory,
    normalizer,
    stabilizer,
    gate,
    up,
    down,
    routes,
    weight,
    memory_next,
    send1,
    recv1,
    recv2,
    send3,
    recv3,
    in_sems,
    out_sem,
    send_sems,
    recv_sems,
):
    rows, width = tokens.shape
    head_size = wq.shape[1]
    quarter = width // n_tp
    n = n_ep * n_tp
    me_e = lax.axis_index("ep")
    me_t = lax.axis_index("tp")
    me = me_e * n_tp + me_t

    sources = (
        tokens_h, gain_mix_h, wq_h, wk_h, wi_h, wf_h, bias_h, stabilizer_h, wv_h, wo_h,
        memory_h, normalizer_h, w_out_h, gain_moe_h, gate_h, up_h, down_h, routes_h, weight_h,
    )
    targets = (
        tokens, gain_mix, wq, wk, wi, wf, bias, stabilizer, wv, wo,
        memory, normalizer, w_out, gain_moe, gate, up, down, routes, weight,
    )
    copies = {}
    for number, (source, target) in enumerate(zip(sources, targets)):
        copy = pltpu.make_async_copy(source, target, in_sems.at[number])
        copy.start()
        copies[id(target)] = copy

    def ready(*refs):
        for ref in refs:
            copies[id(ref)].wait()

    barrier = pltpu.get_barrier_semaphore()

    def greet(step, carry):
        peer = lax.rem(me + step, n)
        pl.semaphore_signal(
            barrier, inc=1, device_id=(peer // n_tp, lax.rem(peer, n_tp)), device_id_type=MESH
        )
        return carry

    lax.fori_loop(1, n, greet, 0)

    ready(tokens, gain_mix)
    values = tokens[...].astype(F32)
    centered = values - jnp.mean(values, -1, keepdims=True)
    variance = jnp.mean(centered * centered, -1, keepdims=True)
    normed = (centered * lax.rsqrt(variance + 1e-05) * gain_mix[...]).astype(BF16)

    def project(ref):
        ready(ref)
        return jnp.dot(normed, ref[...], preferred_element_type=F32).astype(BF16).astype(F32)

    q = project(wq)
    k = project(wk) / math.sqrt(head_size)
    q_cols = q.T
    k_cols = k.T
    ready(wi, wf, bias, stabilizer)
    normed_wide = normed.astype(F32)
    gate_in = jnp.sum(normed_wide * wi[...].astype(F32), -1, keepdims=True)
    gate_forget = jnp.sum(normed_wide * wf[...].astype(F32), -1, keepdims=True)
    biased = gate_forget + bias[...]
    log_forget = jnp.minimum(biased, 0.0) - jnp.log1p(jnp.exp(-jnp.abs(biased)))
    shifted = log_forget + stabilizer[...]
    stab_next = jnp.maximum(shifted, gate_in)
    keep = jnp.exp(shifted - stab_next)
    admit = jnp.exp(gate_in - stab_next)
    v = project(wv)
    o = project(wo)
    ready(memory)
    read = jnp.concatenate(
        [
            jnp.sum(q_cols[:, s : s + 1] * memory[s, 0], axis=0, keepdims=True)
            for s in range(rows)
        ],
        axis=0,
    )
    numerator = keep * read + (admit * jnp.sum(q * k, -1, keepdims=True)) * v
    ready(normalizer)
    norm_next = keep * normalizer[...].reshape(rows, head_size) + admit * k
    denominator = jnp.sum(q * norm_next, -1, keepdims=True)
    readout = numerator / jnp.maximum(jnp.abs(denominator), jnp.exp(-stab_next))
    mixed = (jax.nn.sigmoid(o) * readout).astype(BF16)
    ready(w_out)
    part = jnp.dot(mixed, w_out[...], preferred_element_type=F32)
    for t in range(n_tp):
        send1[t] = part[:, t * quarter : (t + 1) * quarter].astype(BF16)

    pl.semaphore_wait(barrier, n - 1)
    for step in range(1, n_tp):
        peer = lax.rem(me_t + step, n_tp)
        pltpu.make_async_remote_copy(
            src_ref=send1.at[peer],
            dst_ref=recv1.at[me_t],
            send_sem=send_sems.at[0],
            recv_sem=recv_sems.at[0],
            device_id=(me_e, peer),
            device_id_type=MESH,
        ).start()

    norm_out[...] = norm_next.reshape(norm_out.shape)
    stab_out[...] = stab_next
    scaled_cols = k_cols
    for s in range(rows):
        memory_next[s, 0] = keep[s : s + 1] * memory[s, 0] + scaled_cols[:, s : s + 1] * (
            admit[s : s + 1] * v[s : s + 1]
        )
    state_copy = pltpu.make_async_copy(memory_next, memory_out, out_sem)
    state_copy.start()

    def arrived(ref, count, sem):
        pltpu.make_async_copy(ref.at[pl.ds(0, count)], ref.at[pl.ds(0, count)], sem).wait()

    arrived(recv1, n_tp - 1, recv_sems.at[0])
    own = tokens[:, pl.ds(pl.multiple_of(me_t * quarter, quarter), quarter)].astype(F32)
    own = own + send1[me_t].astype(F32)
    for step in range(1, n_tp):
        own = own + recv1[lax.rem(me_t + step, n_tp)].astype(F32)

    recv2[me] = own.astype(BF16)

    def spread(step, carry):
        peer = lax.rem(me + step, n)
        pltpu.make_async_remote_copy(
            src_ref=recv2.at[me],
            dst_ref=recv2.at[me],
            send_sem=send_sems.at[1],
            recv_sem=recv_sems.at[1],
            device_id=(peer // n_tp, lax.rem(peer, n_tp)),
            device_id_type=MESH,
        ).start()
        return carry

    lax.fori_loop(1, n, spread, 0)
    ready(gain_moe, gate, up, down, routes, weight)
    arrived(recv2, n - 1, recv_sems.at[1])

    group = math.gcd(n_ep, 8)
    tall = group * rows

    def expert(index, carry):
        first = index * group
        pieces = []
        for t in range(n_tp):
            piece = jnp.concatenate(
                [recv2[(first + i) * n_tp + t].astype(F32) for i in range(group)], axis=0
            )
            pieces.append(piece)
        mean = sum(jnp.sum(piece, -1, keepdims=True) for piece in pieces) / width
        pieces = [piece - mean for piece in pieces]
        spreads = sum(jnp.sum(piece * piece, -1, keepdims=True) for piece in pieces) / width
        scale = lax.rsqrt(spreads + 1e-05)
        gate_part = jnp.zeros((tall, gate.shape[2]), F32)
        up_part = jnp.zeros((tall, up.shape[2]), F32)
        for t in range(n_tp):
            cut = slice(t * quarter, (t + 1) * quarter)
            rows_in = (pieces[t] * scale * gain_moe[:, cut]).astype(BF16)
            gate_part += jnp.dot(rows_in, gate[0, cut, :], preferred_element_type=F32)
            up_part += jnp.dot(rows_in, up[0, cut, :], preferred_element_type=F32)
        hidden = (jax.nn.silu(gate_part) * up_part).astype(BF16)
        for t in range(n_tp):
            cut = slice(t * quarter, (t + 1) * quarter)
            partial = jnp.dot(hidden, down[0, :, cut], preferred_element_type=F32)
            for i in range(group):
                send3[(first + i) * n_tp + t] = partial[i * rows : (i + 1) * rows].astype(BF16)
        return carry

    if n_ep == group:
        expert(0, 0)
    else:
        lax.fori_loop(0, n_ep // group, expert, 0)

    def home(step, carry):
        peer = lax.rem(me + step, n)
        pltpu.make_async_remote_copy(
            src_ref=send3.at[peer],
            dst_ref=recv3.at[me],
            send_sem=send_sems.at[2],
            recv_sem=recv_sems.at[2],
            device_id=(peer // n_tp, lax.rem(peer, n_tp)),
            device_id_type=MESH,
        ).start()
        return carry

    lax.fori_loop(1, n, home, 0)
    recv3[me] = send3[me]
    arrived(recv3, n - 1, recv_sems.at[2])
    chosen = routes[...]
    shares = weight[...]

    def add_expert(e, total):
        factor = jnp.sum(jnp.where(chosen == e, shares, 0.0), -1, keepdims=True)
        summed = recv3[e * n_tp].astype(F32)
        for t in range(1, n_tp):
            summed = summed + recv3[e * n_tp + t].astype(F32)
        return total + factor * summed

    if n_ep == group:
        for e in range(n_ep):
            own = add_expert(e, own)
    else:
        own = lax.fori_loop(0, n_ep, add_expert, own)
    out_ref[...] = own.astype(BF16)

    arrived(send1, n_tp - 1, send_sems.at[0])
    arrived(recv2, n - 1, send_sems.at[1])
    arrived(send3, n - 1, send_sems.at[2])
    state_copy.wait()


def shards(
    n_ep,
    n_tp,
    tokens,
    w_query,
    w_key,
    w_value,
    w_outgate,
    w_igate,
    w_fgate,
    forget_bias,
    w_out,
    gain_mix,
    gain_moe,
    memory,
    normalizer,
    stabilizer,
    expert_gate,
    expert_up,
    expert_down,
    routes,
    route_weight,
):
    rows, width = tokens.shape
    n = n_ep * n_tp
    quarter = width // n_tp
    assert memory.shape[1] == 1 and expert_gate.shape[0] == 1
    operands = (
        tokens,
        gain_mix.reshape(1, width),
        w_query,
        w_key,
        w_value,
        w_outgate,
        w_igate.reshape(1, width),
        w_fgate.reshape(1, width),
        forget_bias.reshape(1, 1),
        w_out,
        gain_moe.reshape(1, width),
        memory,
        normalizer,
        stabilizer,
        expert_gate,
        expert_up,
        expert_down,
        routes,
        route_weight,
    )
    block = (n, rows, quarter)
    return pl.pallas_call(
        functools.partial(kernel, n_ep, n_tp),
        out_shape=(
            jax.ShapeDtypeStruct((rows, quarter), BF16),
            jax.ShapeDtypeStruct(memory.shape, F32),
            jax.ShapeDtypeStruct(normalizer.shape, F32),
            jax.ShapeDtypeStruct(stabilizer.shape, F32),
        ),
        in_specs=[pl.BlockSpec(memory_space=pl.ANY)] * len(operands),
        out_specs=(
            pl.BlockSpec(memory_space=pltpu.VMEM),
            pl.BlockSpec(memory_space=pl.ANY),
            pl.BlockSpec(memory_space=pltpu.VMEM),
            pl.BlockSpec(memory_space=pltpu.VMEM),
        ),
        scratch_shapes=[pltpu.VMEM(x.shape, x.dtype) for x in operands]
        + [
            pltpu.VMEM(memory.shape, F32),
            pltpu.VMEM((n_tp, rows, quarter), BF16),
            pltpu.VMEM((n_tp, rows, quarter), BF16),
            pltpu.VMEM(block, BF16),
            pltpu.VMEM(block, BF16),
            pltpu.VMEM(block, BF16),
            pltpu.SemaphoreType.DMA((len(operands),)),
            pltpu.SemaphoreType.DMA,
            pltpu.SemaphoreType.DMA((3,)),
            pltpu.SemaphoreType.DMA((3,)),
        ],
        compiler_params=pltpu.CompilerParams(collective_id=0, has_side_effects=True),
        name="cell_and_experts",
    )(*operands)


def solution(mesh):
    return jax.shard_map(
        functools.partial(shards, mesh.shape["ep"], mesh.shape["tp"]),
        mesh=mesh,
        in_specs=(
            P("ep", None),
            P(None, "tp"),
            P(None, "tp"),
            P(None, "tp"),
            P(None, "tp"),
            P(None, "tp"),
            P(None, "tp"),
            P("tp"),
            P("tp", None),
            P(),
            P(),
            P("ep", "tp", None, None),
            P("ep", "tp", None),
            P("ep", "tp"),
            P("ep", None, "tp"),
            P("ep", None, "tp"),
            P("ep", "tp", None),
            P("ep", None),
            P("ep", None),
        ),
        out_specs=(P("ep", "tp"), P("ep", "tp", None, None), P("ep", "tp", None), P("ep", "tp")),
        check_vma=False,
    )
```

```python
import functools
import math

import jax
import jax.numpy as jnp
from jax import lax
from jax.experimental import pallas as pl
from jax.experimental.pallas import tpu as pltpu
from jax.sharding import PartitionSpec as P

MESH = pl.DeviceIdType.MESH
F32 = jnp.float32
BF16 = jnp.bfloat16


def kernel(
    n_ep,
    n_tp,
    tokens_h,
    gain_mix_h,
    wq_h,
    wk_h,
    wv_h,
    wo_h,
    wi_h,
    wf_h,
    bias_h,
    w_out_h,
    gain_moe_h,
    memory_h,
    normalizer_h,
    stabilizer_h,
    gate_h,
    up_h,
    down_h,
    routes_h,
    weight_h,
    pack_ref,
    tokens,
    gain_mix,
    wq,
    wk,
    wv,
    wo,
    wi,
    wf,
    w_out,
    gain_moe,
    memory,
    normalizer,
    stabilizer,
    gate,
    up,
    down,
    routes,
    weight,
    send1,
    recv1,
    recv2,
    give,
    take,
    held,
    send3,
    recv3,
    in_sems,
    send_sems,
    recv_sems,
):
    rows, width = tokens.shape
    head_size = wq.shape[1]
    diagonal = lax.broadcasted_iota(jnp.int32, (rows, rows), 0) == lax.broadcasted_iota(
        jnp.int32, (rows, rows), 1
    )

    def upright(row):
        return jnp.sum(jnp.where(diagonal, row, 0.0), axis=1, keepdims=True)

    def flat(column):
        return jnp.sum(jnp.where(diagonal, column, 0.0), axis=0, keepdims=True)

    quarter = width // n_tp
    n = n_ep * n_tp
    me_e = lax.axis_index("ep")
    me_t = lax.axis_index("tp")
    me = me_e * n_tp + me_t
    pairs = n_tp // 2
    half = n_ep * pairs
    parity = lax.rem(me_t, 2)
    mine = me_e * pairs + me_t // 2
    sibling = (me_e, me_t + 1 - 2 * parity)

    sources = (
        tokens_h, gain_mix_h, wq_h, wk_h, wi_h, wf_h, stabilizer_h, wv_h, wo_h,
        memory_h, normalizer_h, w_out_h, gain_moe_h, gate_h, up_h, down_h, routes_h, weight_h,
    )
    targets = (
        tokens, gain_mix, wq, wk, wi, wf, stabilizer, wv, wo,
        memory, normalizer, w_out, gain_moe, gate, up, down, routes, weight,
    )
    copies = {}
    for number, (source, target) in enumerate(zip(sources, targets)):
        copy = pltpu.make_async_copy(source, target, in_sems.at[number])
        copy.start()
        copies[id(target)] = copy

    def ready(*refs):
        for ref in refs:
            copies[id(ref)].wait()

    barrier = pltpu.get_barrier_semaphore()

    def greet(step, carry):
        peer = lax.rem(me + step, n)
        pl.semaphore_signal(
            barrier, inc=1, device_id=(peer // n_tp, lax.rem(peer, n_tp)), device_id_type=MESH
        )
        return carry

    lax.fori_loop(1, n, greet, 0)

    ready(tokens, gain_mix)
    values = tokens[...].astype(F32)
    centered = values - jnp.mean(values, -1, keepdims=True)
    variance = jnp.mean(centered * centered, -1, keepdims=True)
    normed = (centered * lax.rsqrt(variance + 1e-05) * gain_mix[...]).astype(BF16)

    def project(ref):
        ready(ref)
        return jnp.dot(normed, ref[...], preferred_element_type=F32).astype(BF16).astype(F32)

    q = project(wq)
    k = project(wk) / math.sqrt(head_size)
    q_cols = q.T
    ready(wi, wf, stabilizer)
    normed_wide = normed.astype(F32)
    gate_in = jnp.sum(normed_wide * wi[...].astype(F32), -1, keepdims=True)
    gate_forget = jnp.sum(normed_wide * wf[...].astype(F32), -1, keepdims=True)
    biased = gate_forget + bias_h[0]
    log_forget = jnp.minimum(biased, 0.0) - jnp.log1p(jnp.exp(-jnp.abs(biased)))
    shifted = log_forget + upright(stabilizer[...])
    stab_next = jnp.maximum(shifted, gate_in)
    keep = jnp.exp(shifted - stab_next)
    admit = jnp.exp(gate_in - stab_next)
    v = project(wv)
    o = project(wo)
    ready(memory)
    read = jnp.concatenate(
        [
            jnp.sum(q_cols[:, s : s + 1] * memory[s, 0], axis=0, keepdims=True)
            for s in range(rows)
        ],
        axis=0,
    )
    numerator = keep * read + (admit * jnp.sum(q * k, -1, keepdims=True)) * v
    ready(normalizer)
    norm_next = keep * normalizer[...].reshape(rows, head_size) + admit * k
    denominator = jnp.sum(q * norm_next, -1, keepdims=True)
    readout = numerator / jnp.maximum(jnp.abs(denominator), jnp.exp(-stab_next))
    mixed = (jax.nn.sigmoid(o) * readout).astype(BF16)
    ready(w_out)
    part = jnp.dot(mixed, w_out[...], preferred_element_type=F32)
    for t in range(n_tp):
        send1[t] = part[:, t * quarter : (t + 1) * quarter].astype(BF16)

    pl.semaphore_wait(barrier, n - 1)
    for step in range(1, n_tp):
        peer = lax.rem(me_t + step, n_tp)
        pltpu.make_async_remote_copy(
            src_ref=send1.at[peer],
            dst_ref=recv1.at[me_t],
            send_sem=send_sems.at[0],
            recv_sem=recv_sems.at[0],
            device_id=(me_e, peer),
            device_id_type=MESH,
        ).start()

    lanes = pack_ref.shape[1] - quarter - 3 * head_size
    pack_ref[:, quarter : quarter + head_size] = admit * k
    pack_ref[:, quarter + head_size : quarter + 2 * head_size] = v
    pack_ref[:, quarter + 2 * head_size : quarter + 3 * head_size] = norm_next
    place = lax.broadcasted_iota(jnp.int32, (rows, lanes), 1)
    pack_ref[:, quarter + 3 * head_size :] = jnp.where(place == 0, keep, stab_next)

    def arrived(ref, count, sem):
        pltpu.make_async_copy(ref.at[pl.ds(0, count)], ref.at[pl.ds(0, count)], sem).wait()

    arrived(recv1, n_tp - 1, recv_sems.at[0])
    own = tokens[:, pl.ds(pl.multiple_of(me_t * quarter, quarter), quarter)].astype(F32)
    own = own + send1[me_t].astype(F32)
    for step in range(1, n_tp):
        own = own + recv1[lax.rem(me_t + step, n_tp)].astype(F32)

    recv2[parity * half + mine] = own.astype(BF16)

    def spread(step, carry):
        other = lax.rem(mine + step, half)
        pltpu.make_async_remote_copy(
            src_ref=recv2.at[parity * half + mine],
            dst_ref=recv2.at[parity * half + mine],
            send_sem=send_sems.at[1],
            recv_sem=recv_sems.at[1],
            device_id=(other // pairs, lax.rem(other, pairs) * 2 + parity),
            device_id_type=MESH,
        ).start()
        return carry

    lax.fori_loop(1, half, spread, 0)
    ready(gain_moe, gate, up, down, routes, weight)
    arrived(recv2, half - 1, recv_sems.at[1])
    pltpu.make_async_remote_copy(
        src_ref=recv2.at[pl.ds(parity * half, half)],
        dst_ref=recv2.at[pl.ds(parity * half, half)],
        send_sem=send_sems.at[3],
        recv_sem=recv_sems.at[3],
        device_id=sibling,
        device_id_type=MESH,
    ).start()
    arrived(recv2, half, recv_sems.at[3])

    group = math.gcd(n_ep, 8)
    tall = group * rows

    hand = pltpu.make_async_remote_copy(
        src_ref=give,
        dst_ref=take,
        send_sem=send_sems.at[4],
        recv_sem=recv_sems.at[4],
        device_id=sibling,
        device_id_type=MESH,
    )

    def expert(index, carry):
        first = index * group
        pieces = []
        for t in range(n_tp):
            piece = jnp.concatenate(
                [recv2[(t % 2) * half + (first + i) * pairs + t // 2].astype(F32) for i in range(group)], axis=0
            )
            pieces.append(piece)
        mean = sum(jnp.sum(piece, -1, keepdims=True) for piece in pieces) / width
        pieces = [piece - mean for piece in pieces]
        spreads = sum(jnp.sum(piece * piece, -1, keepdims=True) for piece in pieces) / width
        scale = lax.rsqrt(spreads + 1e-05)
        gate_part = jnp.zeros((tall, gate.shape[2]), F32)
        up_part = jnp.zeros((tall, up.shape[2]), F32)
        for t in range(n_tp):
            cut = slice(t * quarter, (t + 1) * quarter)
            rows_in = (pieces[t] * scale * gain_moe[:, cut]).astype(BF16)
            gate_part += jnp.dot(rows_in, gate[0, cut, :], preferred_element_type=F32)
            up_part += jnp.dot(rows_in, up[0, cut, :], preferred_element_type=F32)
        hidden = (jax.nn.silu(gate_part) * up_part).astype(BF16)

        def partial(t):
            cut = pl.ds(pl.multiple_of(t * quarter, quarter), quarter)
            return jnp.dot(hidden, down[0, :, cut], preferred_element_type=F32)

        for j in range(pairs):
            block = partial(2 * j + 1 - parity)
            for i in range(group):
                give[(first + i) * pairs + j] = block[i * rows : (i + 1) * rows].astype(BF16)
        if n_ep == group:
            hand.start()
        for j in range(pairs):
            block = partial(2 * j + parity)
            for i in range(group):
                held[(first + i) * pairs + j] = block[i * rows : (i + 1) * rows]
        return carry

    if n_ep == group:
        expert(0, 0)
    else:
        lax.fori_loop(0, n_ep // group, expert, 0)
        hand.start()

    arrived(take, half, recv_sems.at[4])

    def pair_sum(index, carry):
        send3[index] = (held[index] + take[index].astype(F32)).astype(BF16)
        return carry

    lax.fori_loop(0, half, pair_sum, 0, unroll=half <= 16)

    def home(step, carry):
        other = lax.rem(mine + step, half)
        pltpu.make_async_remote_copy(
            src_ref=send3.at[other],
            dst_ref=recv3.at[mine],
            send_sem=send_sems.at[2],
            recv_sem=recv_sems.at[2],
            device_id=(other // pairs, lax.rem(other, pairs) * 2 + parity),
            device_id_type=MESH,
        ).start()
        return carry

    lax.fori_loop(1, half, home, 0)
    recv3[mine] = send3[mine]
    arrived(recv3, half - 1, recv_sems.at[2])
    chosen = routes[...]
    shares = weight[...]

    def add_expert(e, total):
        factor = upright(jnp.sum(jnp.where(chosen == e, shares, 0.0), 0, keepdims=True))
        summed = recv3[e * pairs].astype(F32)
        for j in range(1, pairs):
            summed = summed + recv3[e * pairs + j].astype(F32)
        return total + factor * summed

    if n_ep == group:
        for e in range(n_ep):
            own = add_expert(e, own)
    else:
        own = lax.fori_loop(0, n_ep, add_expert, own)
    pack_ref[:, :quarter] = own

    arrived(send1, n_tp - 1, send_sems.at[0])
    arrived(recv2, half - 1, send_sems.at[1])
    arrived(send3, half - 1, send_sems.at[2])
    arrived(recv2, half, send_sems.at[3])
    arrived(give, half, send_sems.at[4])


def finish(pack_h, memory_h, out_h, memory_out, norm_out, stab_out, pack, memory, out, norm, stab, in_sems, out_sems):
    count = memory.shape[0]
    rows, quarter = out.shape
    head_size = memory.shape[2]
    first = pltpu.make_async_copy(pack_h, pack, in_sems.at[count])
    first.start()
    reads = [pltpu.make_async_copy(memory_h.at[s], memory.at[s], in_sems.at[s]) for s in range(count)]
    for read in reads:
        read.start()
    first.wait()
    out[...] = pack[:, :quarter].astype(BF16)
    norm[...] = pack[:, quarter + 2 * head_size : quarter + 3 * head_size].reshape(norm.shape)
    diagonal = lax.broadcasted_iota(jnp.int32, (rows, rows), 0) == lax.broadcasted_iota(
        jnp.int32, (rows, rows), 1
    )
    base = quarter + 3 * head_size
    stab[...] = jnp.sum(jnp.where(diagonal, pack[:, base + 1 : base + 2], 0.0), axis=0, keepdims=True)
    writes = [
        pltpu.make_async_copy(out, out_h, out_sems.at[count]),
        pltpu.make_async_copy(norm, norm_out, out_sems.at[count + 1]),
        pltpu.make_async_copy(stab, stab_out, out_sems.at[count + 2]),
    ]
    for write in writes:
        write.start()
    k_cols = pack[:, quarter : quarter + head_size].T
    v = pack[:, quarter + head_size : quarter + 2 * head_size]
    keep = pack[:, base : base + 1]
    for s in range(count):
        reads[s].wait()
        memory[s, 0] = keep[s : s + 1] * memory[s, 0] + k_cols[:, s : s + 1] * v[s : s + 1]
        write = pltpu.make_async_copy(memory.at[s], memory_out.at[s], out_sems.at[s])
        write.start()
        writes.append(write)
    for write in writes:
        write.wait()


def shards(
    n_ep,
    n_tp,
    tokens,
    w_query,
    w_key,
    w_value,
    w_outgate,
    w_igate,
    w_fgate,
    forget_bias,
    w_out,
    gain_mix,
    gain_moe,
    memory,
    normalizer,
    stabilizer,
    expert_gate,
    expert_up,
    expert_down,
    routes,
    route_weight,
):
    rows, width = tokens.shape
    n = n_ep * n_tp
    quarter = width // n_tp
    assert memory.shape[1] == 1 and expert_gate.shape[0] == 1
    operands = (
        tokens,
        gain_mix.reshape(1, width),
        w_query,
        w_key,
        w_value,
        w_outgate,
        w_igate.reshape(1, width),
        w_fgate.reshape(1, width),
        forget_bias,
        w_out,
        gain_moe.reshape(1, width),
        memory,
        normalizer,
        stabilizer.T,
        expert_gate,
        expert_up,
        expert_down,
        routes.T,
        route_weight.T,
    )
    block = (n, rows, quarter)
    half = (n // 2, rows, quarter)
    head_size = memory.shape[2]
    pack_width = quarter + 3 * head_size + 128
    pack = pl.pallas_call(
        functools.partial(kernel, n_ep, n_tp),
        out_shape=jax.ShapeDtypeStruct((rows, pack_width), F32),
        in_specs=[
            pl.BlockSpec(memory_space=pltpu.SMEM if x is forget_bias else pl.ANY) for x in operands
        ],
        out_specs=pl.BlockSpec(memory_space=pltpu.VMEM),
        scratch_shapes=[pltpu.VMEM(x.shape, x.dtype) for x in operands if x is not forget_bias]
        + [
            pltpu.VMEM((n_tp, rows, quarter), BF16),
            pltpu.VMEM((n_tp, rows, quarter), BF16),
            pltpu.VMEM(block, BF16),
            pltpu.VMEM(half, BF16),
            pltpu.VMEM(half, BF16),
            pltpu.VMEM(half, F32),
            pltpu.VMEM(half, BF16),
            pltpu.VMEM(half, BF16),
            pltpu.SemaphoreType.DMA((len(operands),)),
            pltpu.SemaphoreType.DMA((5,)),
            pltpu.SemaphoreType.DMA((5,)),
        ],
        compiler_params=pltpu.CompilerParams(collective_id=0, has_side_effects=True),
        name="cell_and_experts",
    )(*operands)
    results = (
        jax.ShapeDtypeStruct((rows, quarter), BF16),
        jax.ShapeDtypeStruct(memory.shape, F32),
        jax.ShapeDtypeStruct(normalizer.shape, F32),
        jax.ShapeDtypeStruct((1, rows), F32),
    )
    out, memory_next, norm_next, stab_row = pl.pallas_call(
        finish,
        out_shape=results,
        in_specs=[pl.BlockSpec(memory_space=pl.ANY)] * 2,
        out_specs=[pl.BlockSpec(memory_space=pl.ANY)] * 4,
        scratch_shapes=[
            pltpu.VMEM((rows, pack_width), F32),
            pltpu.VMEM(memory.shape, F32),
            pltpu.VMEM((rows, quarter), BF16),
            pltpu.VMEM(normalizer.shape, F32),
            pltpu.VMEM((1, rows), F32),
            pltpu.SemaphoreType.DMA((rows + 1,)),
            pltpu.SemaphoreType.DMA((rows + 3,)),
        ],
        name="state",
    )(pack, memory)
    return out, memory_next, norm_next, stab_row.T


def solution(mesh):
    return jax.shard_map(
        functools.partial(shards, mesh.shape["ep"], mesh.shape["tp"]),
        mesh=mesh,
        in_specs=(
            P("ep", None),
            P(None, "tp"),
            P(None, "tp"),
            P(None, "tp"),
            P(None, "tp"),
            P(None, "tp"),
            P(None, "tp"),
            P("tp"),
            P("tp", None),
            P(),
            P(),
            P("ep", "tp", None, None),
            P("ep", "tp", None),
            P("ep", "tp"),
            P("ep", None, "tp"),
            P("ep", None, "tp"),
            P("ep", "tp", None),
            P("ep", None),
            P("ep", None),
        ),
        out_specs=(P("ep", "tp"), P("ep", "tp", None, None), P("ep", "tp", None), P("ep", "tp")),
        check_vma=False,
    )
```
